32 devices in a mesh: rep: 2 (over core), fs: 8 (over z, y), tp: 2 (over x).
Axes of the slice: x: 2, y: 2, z: 4, core: 2. Of those that a mesh axis runs over, the one named last changes fastest.
Arguments:
- tokens: bfloat16 [16, 768, 2048], P(('rep', 'fs')), may hold values from -6 to 6
- mixer_gain: float32 [2048], replicated, may hold values from 0.1 to 1.9
- value_weight: float32 [2048, 4, 512], P('fs', None, 'tp'), may hold values from -0.125 to 0.125
- value_scale: float32 [4, 512], P(None, 'tp'), may hold values from 0.5 to 2
- gate_weight: float32 [2048, 4, 512], P('fs', None, 'tp'), may hold values from -0.125 to 0.125
- gate_scale: float32 [4, 512], P(None, 'tp'), may hold values from 0.5 to 2
- pool_weight: float32 [4, 512, 512], P(None, 'fs', 'tp'), may hold values from -0.25 to 0.25
- pool_scale: float32 [4, 512], P(None, 'tp'), may hold values from 0.5 to 2
- channel_gain: float32 [2048], replicated, may hold values from 0.1 to 1.9
- up_weight: float32 [2048, 4096], P('fs', 'tp'), may hold values from -0.125 to 0.125
- up_scale: float32 [4096], P('tp'), may hold values from 0.5 to 2
- down_weight: float32 [4096, 2048], P('tp', 'fs'), may hold values from -0.09375 to 0.09375
- down_scale: float32 [2048], P('fs'), may hold values from 0.5 to 2
Outputs:
- layer_out: bfloat16 [16, 768, 2048], P(('rep', 'fs'), 'tp')
The draws below stay inside these ranges and needn't reach their ends.
All inputs are finite; a program needn't handle non-finite values.
Results may differ from the reference program's by a relative error of at most 0.015.
Values may be sent and summed in bfloat16 or wider, within the bound.
A program may use at most 64 MiB of HBM per device.

```python
import math
import jax
import jax.numpy as jnp
from jax import lax

D = 2048
GROUPS = 4
GROUP_WIDTH = 512
FF = 4096
SEQ_LEN = 768
SEQS = 16
N_TP = 2


def levels(rng, dims, pieces, low, high):
    loudness, own = 1.0, jax.random.fold_in(rng, 6)
    for dim, parts in pieces:
        steps = jnp.exp(jax.random.uniform(jax.random.fold_in(own, dim), (parts,), jnp.float32, low / len(pieces), high / len(pieces)))
        loudness = loudness * jnp.repeat(steps, dims[dim] // parts).reshape([-1 if axis == dim else 1 for axis in range(len(dims))])
    return loudness


def normal_values(own_key, dims, scale, limit, shards=(), dtype=jnp.bfloat16):
    loudness = levels(own_key, dims, shards, -0.22, 0.18) if shards else 1.0
    values = jax.random.normal(own_key, dims, jnp.float32) * scale * loudness
    return jnp.minimum(jnp.maximum(values, -limit), limit).astype(dtype)


def setup_inputs(seed: int = 0) -> dict:
    seeds = jax.random.split(jax.random.key(seed), 14)
    tokens = normal_values(seeds[0], (SEQS, SEQ_LEN, D), 1.0, 6.0, ((0, 16),))
    mixer_gain = jnp.clip(1.0 + 0.18 * jax.random.normal(seeds[1], (D,), jnp.float32), 0.1, 1.9)
    value_weight = normal_values(seeds[2], (D, GROUPS, GROUP_WIDTH), D ** -0.5, 0.125, ((0, 8), (2, 2)), jnp.float32)
    value_scale = jnp.clip(jnp.exp(math.log(2.0) - 1.3862944 * jax.random.uniform(seeds[3], (GROUPS, GROUP_WIDTH), jnp.float32) ** levels(seeds[3], (GROUPS, GROUP_WIDTH), ((1, 2),), -0.2, 0.2)), 0.5, 2.0)
    gate_weight = normal_values(seeds[4], (D, GROUPS, GROUP_WIDTH), D ** -0.5, 0.125, ((0, 8), (2, 2)), jnp.float32)
    gate_scale = jnp.clip(jnp.exp(math.log(2.0) - 1.3862944 * jax.random.uniform(seeds[5], (GROUPS, GROUP_WIDTH), jnp.float32) ** levels(seeds[5], (GROUPS, GROUP_WIDTH), ((1, 2),), -0.2, 0.2)), 0.5, 2.0)
    pool_weight = normal_values(seeds[6], (GROUPS, GROUP_WIDTH, GROUP_WIDTH), GROUP_WIDTH ** -0.5, 0.25, ((1, 8), (2, 2)), jnp.float32)
    pool_scale = jnp.clip(jnp.exp(math.log(2.0) - 1.3862944 * jax.random.uniform(seeds[7], (GROUPS, GROUP_WIDTH), jnp.float32) ** levels(seeds[7], (GROUPS, GROUP_WIDTH), ((1, 2),), -0.2, 0.2)), 0.5, 2.0)
    channel_gain = jnp.clip(1.0 + 0.18 * jax.random.normal(seeds[8], (D,), jnp.float32), 0.1, 1.9)
    up_weight = normal_values(seeds[9], (D, FF), D ** -0.5, 0.125, ((0, 8), (1, 2)), jnp.float32)
    up_scale = jnp.clip(jnp.exp(math.log(2.0) - 1.3862944 * jax.random.uniform(seeds[10], (FF,), jnp.float32) ** levels(seeds[10], (FF,), ((0, 2),), -0.2, 0.2)), 0.5, 2.0)
    down_weight = normal_values(seeds[11], (FF, D), FF ** -0.5, 0.09375, ((0, 2), (1, 8)), jnp.float32)
    down_scale = jnp.clip(jnp.exp(math.log(2.0) - 1.3862944 * jax.random.uniform(seeds[12], (D,), jnp.float32) ** levels(seeds[12], (D,), ((0, 8),), -0.2, 0.2)), 0.5, 2.0)
    return dict(tokens=tokens, mixer_gain=mixer_gain, value_weight=value_weight, value_scale=value_scale, gate_weight=gate_weight, gate_scale=gate_scale, pool_weight=pool_weight, pool_scale=pool_scale, channel_gain=channel_gain, up_weight=up_weight, up_scale=up_scale, down_weight=down_weight, down_scale=down_scale)


def norm_rows(values, gain):
    floats = values.astype(jnp.float32)
    return floats * lax.rsqrt(lax.optimization_barrier(jnp.mean(floats * floats, axis=-1, keepdims=True)) + 1e-06) * gain

def pool_excess(value):
    floats = value.astype(jnp.float32)
    seq_length = floats.shape[1]
    running = floats
    results = []
    for group in range(floats.shape[2]):
        span = 2 ** group
        shifted = jnp.pad(running, ((0, 0), (span, 0), (0, 0), (0, 0)))[:, :seq_length]
        running = running + shifted
        counts = jnp.minimum(jnp.arange(1, seq_length + 1), 2 * span).astype(jnp.float32)
        results.append(running[:, :, group, :] / counts[None, :, None] - floats[:, :, group, :])
    return jnp.stack(results, axis=2)

def rounded(values):
    return lax.optimization_barrier(values.astype(jnp.bfloat16)).astype(jnp.float32)

def reference(tokens, mixer_gain, value_weight, value_scale, gate_weight, gate_scale, pool_weight, pool_scale, channel_gain, up_weight, up_scale, down_weight, down_scale):
    seq_count, seq_length, model_width = tokens.shape
    row_count = seq_count * seq_length
    normed = norm_rows(tokens, mixer_gain).astype(jnp.bfloat16).reshape(row_count, model_width)
    value = jnp.dot(normed, value_weight.astype(jnp.bfloat16).reshape(model_width, -1), preferred_element_type=jnp.float32)
    value = (value * value_scale.reshape(-1)).astype(jnp.bfloat16).reshape(seq_count, seq_length, GROUPS, GROUP_WIDTH)
    gate = jnp.dot(normed, gate_weight.astype(jnp.bfloat16).reshape(model_width, -1), preferred_element_type=jnp.float32)
    gate = (gate * gate_scale.reshape(-1)).reshape(seq_count, seq_length, GROUPS, GROUP_WIDTH)
    excess = pool_excess(value).astype(jnp.bfloat16)
    pooled = jnp.einsum('slgc,gce->slge', excess.astype(jnp.float32), pool_weight.astype(jnp.bfloat16).astype(jnp.float32)) * pool_scale
    merged = (jax.nn.sigmoid(gate) * pooled).astype(jnp.bfloat16)
    middle = tokens.reshape(row_count, model_width).astype(jnp.float32) + merged.reshape(row_count, model_width).astype(jnp.float32)
    normed_two = norm_rows(middle, channel_gain).astype(jnp.bfloat16)
    upward = jnp.dot(normed_two, up_weight.astype(jnp.bfloat16), preferred_element_type=jnp.float32) * up_scale
    hidden = jnp.square(jax.nn.relu(upward)).astype(jnp.bfloat16)
    down_matrix = down_weight.astype(jnp.bfloat16)
    hidden_block = FF // N_TP
    summed = jnp.zeros((row_count, model_width), jnp.float32)
    for member in range(N_TP):
        part = hidden[:, member * hidden_block:(member + 1) * hidden_block]
        rows_part = down_matrix[member * hidden_block:(member + 1) * hidden_block]
        summed = summed + rounded(jnp.dot(part, rows_part, preferred_element_type=jnp.float32) * down_scale)
    return (middle + summed).astype(jnp.bfloat16).reshape(seq_count, seq_length, model_width)
```

```python
import functools

import jax
import jax.numpy as jnp
from jax import lax
from jax.experimental import pallas as pl
from jax.experimental.pallas import tpu as pltpu
from jax.sharding import PartitionSpec as P

NY = 2
UP, DOWN, ACROSS, SIBLING = range(4)


class Gather:
    def __init__(self, sizes, srcs, fulls, axes, send_sem, recv_sem, local_sem):
        self.nf = sizes["fs"]
        self.nz = self.nf // NY
        self.rep, self.place, self.tp = lax.axis_index("rep"), lax.axis_index("fs"), lax.axis_index("tp")
        self.z, self.y = self.place // NY, self.place % NY
        self.srcs, self.fulls, self.axes = srcs, fulls, axes
        self.send_sem, self.recv_sem, self.local_sem = send_sem, recv_sem, local_sem

    def target(self, way):
        rep, place = self.rep, self.place
        if way == UP:
            place = place + NY
        elif way == DOWN:
            place = place - NY
        elif way == ACROSS:
            place = self.z * NY + 1 - self.y
        else:
            rep = 1 - rep
        return {"rep": rep, "fs": place, "tp": self.tp}

    def view(self, ref, w, start, size):
        axis = self.axes[w]
        return ref.at[tuple([slice(None)] * axis + [pl.ds(start, size)])]

    def piece(self, w, k, half):
        rows = self.srcs[w].shape[self.axes[w]]
        part = rows // 2
        start = pl.multiple_of(k * rows + half * part, part)
        return self.view(self.fulls[w], w, start, part)

    def own_piece(self, w):
        part = self.srcs[w].shape[self.axes[w]] // 2
        return self.view(self.srcs[w], w, pl.multiple_of(self.rep * part, part), part)

    def copy(self, w, k, way, own=False, half=None):
        half = self.rep if half is None else half
        return pltpu.make_async_remote_copy(
            src_ref=self.own_piece(w) if own else self.piece(w, k, half),
            dst_ref=self.piece(w, k, half),
            send_sem=self.send_sem.at[way, w, k],
            recv_sem=self.recv_sem.at[1 if way == SIBLING else 0, w, k],
            device_id=self.target(way),
            device_id_type=pl.DeviceIdType.MESH,
        )

    def barrier(self, others=()):
        sem = pltpu.get_barrier_semaphore()

        def greet(device):
            pl.semaphore_signal(sem, inc=1, device_id=device, device_id_type=pl.DeviceIdType.MESH)

        for way in (ACROSS, SIBLING):
            greet(self.target(way))
        for device in others:
            greet(device)
        pl.when(self.z > 0)(lambda: greet(self.target(DOWN)))
        pl.when(self.z < self.nz - 1)(lambda: greet(self.target(UP)))
        ends = (self.z > 0).astype(jnp.int32) + (self.z < self.nz - 1).astype(jnp.int32)
        pl.semaphore_wait(sem, 2 + len(others) + ends)

    def local(self, w):
        rows = self.srcs[w].shape[self.axes[w]]
        return pltpu.make_async_copy(
            self.srcs[w], self.view(self.fulls[w], w, pl.multiple_of(self.place * rows, rows), rows), self.local_sem.at[w]
        )

    def own(self, w):
        pl.when(self.z < self.nz - 1)(lambda: self.copy(w, self.place, UP, own=True).start())
        pl.when(self.z > 0)(lambda: self.copy(w, self.place, DOWN, own=True).start())
        self.copy(w, self.place, ACROSS, own=True).start()

    def pass_on(self, w, k, ways):
        self.copy(w, k, ACROSS).wait_recv()
        for way in ways:
            if way == UP:
                pl.when(self.z < self.nz - 1)(lambda: self.copy(w, k, UP).start())
            elif way == DOWN:
                pl.when(self.z > 0)(lambda: self.copy(w, k, DOWN).start())
            else:
                self.copy(w, k, way).start()

    def along(self, w, d):
        pl.when(self.z >= d)(lambda: self.pass_on(w, (self.z - d) * NY + self.y, (UP, ACROSS, SIBLING)))
        pl.when(self.z + d < self.nz)(lambda: self.pass_on(w, (self.z + d) * NY + self.y, (DOWN, ACROSS, SIBLING)))

    def across(self, w, d):
        other = 1 - self.y
        pl.when(self.z >= d)(lambda: self.pass_on(w, (self.z - d) * NY + other, (SIBLING,)))
        if d:
            pl.when(self.z + d < self.nz)(lambda: self.pass_on(w, (self.z + d) * NY + other, (SIBLING,)))

    def ready(self, w):
        self.local(w).wait()

        @pl.loop(0, self.nf)
        def _(k):
            pl.when(k != self.place)(lambda: self.copy(w, k, SIBLING, half=1 - self.rep).wait_recv())

    def drain(self):
        for w in range(len(self.srcs)):

            @pl.loop(0, self.nf)
            def _(k):
                z, y = k // NY, k % NY
                mine = y == self.y
                pl.when(mine & (z <= self.z) & (self.z < self.nz - 1))(lambda: self.copy(w, k, UP).wait_send())
                pl.when(mine & (z >= self.z) & (self.z > 0))(lambda: self.copy(w, k, DOWN).wait_send())
                pl.when(mine)(lambda: self.copy(w, k, ACROSS).wait_send())
                pl.when(k != self.place)(lambda: self.copy(w, k, SIBLING).wait_send())


def gather_kernel(sizes, axes, *refs):
    count = len(axes)
    g = Gather(sizes, refs[:count], refs[count : 2 * count], axes, *refs[2 * count :])
    for w in range(count):
        g.local(w).start()
    g.barrier()
    g.own(0)
    for w in range(count):
        for d in range(1, g.nz):
            g.along(w, d)
            if d == 1 and w + 1 < count:
                g.own(w + 1)
            if w:
                g.across(w - 1, d - 1)
        if w:
            g.across(w - 1, g.nz - 1)
    for d in range(g.nz):
        g.across(count - 1, d)
    for w in range(count):
        g.ready(w)
    g.drain()


def gather_all(sizes, weights, axes):
    fulls = []
    for weight, axis in zip(weights, axes):
        shape = list(weight.shape)
        shape[axis] *= sizes["fs"]
        fulls.append(jax.ShapeDtypeStruct(tuple(shape), weight.dtype))
    count = len(weights)
    return pl.pallas_call(
        functools.partial(gather_kernel, sizes, axes),
        out_shape=fulls,
        in_specs=[pl.BlockSpec(memory_space=pltpu.VMEM)] * count,
        out_specs=[pl.BlockSpec(memory_space=pl.ANY)] * count,
        scratch_shapes=[
            pltpu.SemaphoreType.DMA((4, count, sizes["fs"])),
            pltpu.SemaphoreType.DMA((2, count, sizes["fs"])),
            pltpu.SemaphoreType.DMA((count,)),
        ],
        compiler_params=pltpu.CompilerParams(collective_id=0, has_side_effects=True),
    )(*weights)


def norm_rows(values, gain):
    floats = values.astype(jnp.float32)
    return floats * lax.rsqrt(jnp.mean(floats * floats, axis=-1, keepdims=True) + 1e-06) * gain


def pool_excess(value):
    floats = value.astype(jnp.float32)
    seq_length = floats.shape[1]
    running = floats
    results = []
    for group in range(floats.shape[2]):
        span = 2**group
        shifted = jnp.pad(running, ((0, 0), (span, 0), (0, 0), (0, 0)))[:, :seq_length]
        running = running + shifted
        counts = jnp.minimum(jnp.arange(1, seq_length + 1), 2 * span).astype(jnp.float32)
        results.append(running[:, :, group, :] / counts[None, :, None] - floats[:, :, group, :])
    return jnp.stack(results, axis=2)


def per_device(
    tokens,
    mixer_gain,
    value_weight,
    value_scale,
    gate_weight,
    gate_scale,
    pool_weight,
    pool_scale,
    channel_gain,
    up_weight,
    up_scale,
    down_weight,
    down_scale,
):
    seq_count, seq_length, model_width = tokens.shape
    shares = lax.axis_size("tp")
    member = lax.axis_index("tp")
    kept_rows = seq_length // shares
    row_count = seq_count * seq_length
    group_count, local_width = value_scale.shape
    value_full, gate_full, pool_full = (
        lax.all_gather(value_weight.astype(jnp.bfloat16), "fs", axis=0, tiled=True),
        lax.all_gather(gate_weight.astype(jnp.bfloat16), "fs", axis=0, tiled=True),
        lax.all_gather(pool_weight.astype(jnp.bfloat16), "fs", axis=1, tiled=True),
    )
    down_scales = lax.all_gather(down_scale, "fs", axis=0, tiled=True)
    normed = norm_rows(tokens, mixer_gain).astype(jnp.bfloat16).reshape(row_count, model_width)
    value = jnp.dot(normed, value_full.reshape(model_width, -1), preferred_element_type=jnp.float32)
    value = (
        (value * value_scale.reshape(-1))
        .astype(jnp.bfloat16)
        .reshape(seq_count, seq_length, group_count, local_width)
    )
    gating = jnp.dot(normed, gate_full.reshape(model_width, -1), preferred_element_type=jnp.float32)
    gating = (gating * gate_scale.reshape(-1)).reshape(
        seq_count, seq_length, group_count, local_width
    )
    excess = pool_excess(value).astype(jnp.bfloat16)
    rows_part = pool_full
    pooled = jnp.einsum(
        "slgc,gce->slge",
        lax.all_gather(excess, "tp", axis=3, tiled=True),
        rows_part,
        preferred_element_type=jnp.float32,
    )
    merged = (jax.nn.sigmoid(gating) * (pooled * pool_scale)).astype(jnp.bfloat16)
    merged_own = lax.all_to_all(merged, "tp", split_axis=1, concat_axis=3, tiled=True)
    own_rows = lax.dynamic_slice_in_dim(tokens, member * kept_rows, kept_rows, 1)
    middle = own_rows.reshape(seq_count * kept_rows, model_width).astype(
        jnp.float32
    ) + merged_own.reshape(seq_count * kept_rows, model_width).astype(jnp.float32)
    normed_two = norm_rows(middle, channel_gain).astype(jnp.bfloat16)
    up_full, down_full = (
        lax.all_gather(up_weight.astype(jnp.bfloat16), "fs", axis=0, tiled=True),
        lax.all_gather(down_weight.astype(jnp.bfloat16), "fs", axis=1, tiled=True),
    )
    upward = (
        jnp.dot(
            lax.all_gather(normed_two, "tp", axis=0, tiled=True),
            up_full,
            preferred_element_type=jnp.float32,
        )
        * up_scale
    )
    hidden = jnp.square(jax.nn.relu(upward)).astype(jnp.bfloat16)
    rows_part = hidden
    summed = lax.psum_scatter(
        (jnp.dot(rows_part, down_full, preferred_element_type=jnp.float32) * down_scales).astype(
            jnp.bfloat16
        ),
        "tp",
        scatter_dimension=0,
        tiled=True,
    ).astype(jnp.float32)
    return (middle + summed).astype(jnp.bfloat16).reshape(seq_count, kept_rows, model_width)


def swap(values):
    other = lax.ppermute(values, "tp", [(0, 1), (1, 0)])
    first = lax.axis_index("tp") == 0
    return jnp.stack([jnp.where(first, values, other), jnp.where(first, other, values)])


def paired_device(
    sizes,
    tokens,
    mixer_gain,
    value_weight,
    value_scale,
    gate_weight,
    gate_scale,
    pool_weight,
    pool_scale,
    channel_gain,
    up_weight,
    up_scale,
    down_weight,
    down_scale,
):
    seq_count, seq_length, model_width = tokens.shape
    shares = lax.axis_size("tp")
    member = lax.axis_index("tp")
    kept_rows = seq_length // shares
    group_count, local_width = value_scale.shape
    rows = value_weight.shape[0]
    value_full, gate_full, pool_full, up_full, down_full = gather_all(
        sizes,
        (
            value_weight.astype(jnp.bfloat16).reshape(rows, -1),
            gate_weight.astype(jnp.bfloat16).reshape(rows, -1),
            pool_weight.astype(jnp.bfloat16),
            up_weight.astype(jnp.bfloat16),
            down_weight.astype(jnp.bfloat16).T,
        ),
        (0, 0, 1, 0, 0),
    )
    down_scales = lax.all_gather(down_scale, "fs", axis=0, tiled=True)
    outs = []
    for tokens_here in tokens:
        normed = norm_rows(tokens_here, mixer_gain).astype(jnp.bfloat16)
        value = jnp.dot(normed, value_full, preferred_element_type=jnp.float32)
        value = (value * value_scale.reshape(-1)).astype(jnp.bfloat16)
        gating = jnp.dot(normed, gate_full, preferred_element_type=jnp.float32) * gate_scale.reshape(-1)
        excess = pool_excess(value.reshape(1, seq_length, group_count, local_width)).astype(jnp.bfloat16)
        both = swap(excess[0].reshape(seq_length, -1))
        merged = []
        for group in range(group_count):
            cut = slice(group * local_width, (group + 1) * local_width)
            pooled = jnp.dot(
                jnp.concatenate([both[i][:, cut] for i in range(shares)], axis=1),
                pool_full[group],
                preferred_element_type=jnp.float32,
            )
            merged.append((jax.nn.sigmoid(gating[:, cut]) * (pooled * pool_scale[group])).astype(jnp.bfloat16))
        merged = swap(jnp.concatenate(merged, axis=1))
        merged = jnp.concatenate(
            [
                merged[i][:, group * local_width : (group + 1) * local_width]
                for group in range(group_count)
                for i in range(shares)
            ],
            axis=1,
        )
        middle = tokens_here.astype(jnp.float32) + merged.astype(jnp.float32)
        normed_two = norm_rows(middle, channel_gain).astype(jnp.bfloat16)
        upward = jnp.dot(normed_two, up_full, preferred_element_type=jnp.float32) * up_scale
        hidden = jnp.square(jax.nn.relu(upward)).astype(jnp.bfloat16)
        part = (
            lax.dot_general(hidden, down_full, (((1,), (1,)), ((), ())), preferred_element_type=jnp.float32)
            * down_scales
        ).astype(jnp.bfloat16)
        theirs = lax.dynamic_slice_in_dim(part, (1 - member) * kept_rows, kept_rows, 0)
        mine = lax.dynamic_slice_in_dim(part, member * kept_rows, kept_rows, 0)
        got = lax.ppermute(theirs, "tp", [(0, 1), (1, 0)])
        summed = mine.astype(jnp.float32) + got.astype(jnp.float32)
        own = lax.dynamic_slice_in_dim(middle, member * kept_rows, kept_rows, 0)
        outs.append((own + summed).astype(jnp.bfloat16))
    return jnp.stack(outs)


def solution(mesh):
    sizes = dict(mesh.shape)
    paired = sizes["rep"] == 2 and sizes["tp"] == 2 and sizes["fs"] % NY == 0 and sizes["fs"] <= 16
    return jax.shard_map(
        functools.partial(paired_device, sizes) if paired else per_device,
        mesh=mesh,
        in_specs=(
            P(("rep", "fs"), None, None),
            P(),
            P("fs", None, "tp"),
            P(None, "tp"),
            P("fs", None, "tp"),
            P(None, "tp"),
            P(None, "fs", "tp"),
            P(None, "tp"),
            P(),
            P("fs", "tp"),
            P("tp"),
            P("tp", "fs"),
            P("fs"),
        ),
        out_specs=P(("rep", "fs"), "tp", None),
        check_vma=False,
    )
```

```python
import functools

import jax
import jax.numpy as jnp
from jax import lax
from jax.experimental import pallas as pl
from jax.experimental.pallas import tpu as pltpu
from jax.sharding import PartitionSpec as P

NY = 2
UP, DOWN, ACROSS, SIBLING = range(4)


class Gather:
    def __init__(self, sizes, srcs, fulls, axes, send_sem, recv_sem, local_sem):
        self.nf = sizes["fs"]
        self.nz = self.nf // NY
        self.rep, self.place, self.tp = lax.axis_index("rep"), lax.axis_index("fs"), lax.axis_index("tp")
        self.z, self.y = self.place // NY, self.place % NY
        self.srcs, self.fulls, self.axes = srcs, fulls, axes
        self.send_sem, self.recv_sem, self.local_sem = send_sem, recv_sem, local_sem

    def target(self, way):
        rep, place = self.rep, self.place
        if way == UP:
            place = place + NY
        elif way == DOWN:
            place = place - NY
        elif way == ACROSS:
            place = self.z * NY + 1 - self.y
        else:
            rep = 1 - rep
        return {"rep": rep, "fs": place, "tp": self.tp}

    def view(self, ref, w, start, size):
        axis = self.axes[w]
        return ref.at[tuple([slice(None)] * axis + [pl.ds(start, size)])]

    def piece(self, w, k, half):
        rows = self.srcs[w].shape[self.axes[w]]
        part = rows // 2
        start = pl.multiple_of(k * rows + half * part, part)
        return self.view(self.fulls[w], w, start, part)

    def copy(self, w, k, way, half=None):
        half = self.rep if half is None else half
        return pltpu.make_async_remote_copy(
            src_ref=self.piece(w, k, half),
            dst_ref=self.piece(w, k, half),
            send_sem=self.send_sem.at[way, w, k],
            recv_sem=self.recv_sem.at[1 if way == SIBLING else 0, w, k],
            device_id=self.target(way),
            device_id_type=pl.DeviceIdType.MESH,
        )

    def barrier(self, others=()):
        sem = pltpu.get_barrier_semaphore()

        def greet(device):
            pl.semaphore_signal(sem, inc=1, device_id=device, device_id_type=pl.DeviceIdType.MESH)

        for way in (ACROSS, SIBLING):
            greet(self.target(way))
        for device in others:
            greet(device)
        pl.when(self.z > 0)(lambda: greet(self.target(DOWN)))
        pl.when(self.z < self.nz - 1)(lambda: greet(self.target(UP)))
        ends = (self.z > 0).astype(jnp.int32) + (self.z < self.nz - 1).astype(jnp.int32)
        pl.semaphore_wait(sem, 2 + len(others) + ends)

    def local(self, w):
        rows = self.srcs[w].shape[self.axes[w]]
        return pltpu.make_async_copy(
            self.srcs[w], self.view(self.fulls[w], w, pl.multiple_of(self.place * rows, rows), rows), self.local_sem.at[w]
        )

    def own(self, w):
        pl.when(self.z < self.nz - 1)(lambda: self.copy(w, self.place, UP).start())
        pl.when(self.z > 0)(lambda: self.copy(w, self.place, DOWN).start())
        self.copy(w, self.place, ACROSS).start()

    def pass_on(self, w, k, ways):
        self.copy(w, k, ACROSS).wait_recv()
        for way in ways:
            if way == UP:
                pl.when(self.z < self.nz - 1)(lambda: self.copy(w, k, UP).start())
            elif way == DOWN:
                pl.when(self.z > 0)(lambda: self.copy(w, k, DOWN).start())
            else:
                self.copy(w, k, way).start()

    def along(self, w, d):
        pl.when(self.z >= d)(lambda: self.pass_on(w, (self.z - d) * NY + self.y, (UP, ACROSS, SIBLING)))
        pl.when(self.z + d < self.nz)(lambda: self.pass_on(w, (self.z + d) * NY + self.y, (DOWN, ACROSS, SIBLING)))

    def across(self, w, d):
        other = 1 - self.y
        pl.when(self.z >= d)(lambda: self.pass_on(w, (self.z - d) * NY + other, (SIBLING,)))
        if d:
            pl.when(self.z + d < self.nz)(lambda: self.pass_on(w, (self.z + d) * NY + other, (SIBLING,)))

    def ready(self, w):
        @pl.loop(0, self.nf)
        def _(k):
            pl.when(k != self.place)(lambda: self.copy(w, k, SIBLING, half=1 - self.rep).wait_recv())

    def drain(self):
        for w in range(len(self.srcs)):

            @pl.loop(0, self.nf)
            def _(k):
                z, y = k // NY, k % NY
                mine = y == self.y
                pl.when(mine & (z <= self.z) & (self.z < self.nz - 1))(lambda: self.copy(w, k, UP).wait_send())
                pl.when(mine & (z >= self.z) & (self.z > 0))(lambda: self.copy(w, k, DOWN).wait_send())
                pl.when(mine)(lambda: self.copy(w, k, ACROSS).wait_send())
                pl.when(k != self.place)(lambda: self.copy(w, k, SIBLING).wait_send())


VALUE, GATE, POOL, SCALES, HIDE, SHOW = range(6)
AXES = (0, 0, 1, 0, 0, 0)


def layer_kernel(sizes, *refs):
    count = len(AXES)
    tokens, mixer_gain, value_scale, gate_scale, pool_scale, channel_gain, up_scale = refs[:7]
    srcs, out, fulls = refs[7 : 7 + count], refs[7 + count], refs[8 + count : 8 + 2 * count]
    normed, excess, excess_in, gate, merged, merged_in, hidden, part_out, part_own, part_in = refs[
        8 + 2 * count : 18 + 2 * count
    ]
    send_sem, recv_sem, local_sem, pair_send, pair_recv = refs[18 + 2 * count :]
    g = Gather(sizes, srcs, fulls, AXES, send_sem, recv_sem, local_sem)
    rows, width = tokens.shape
    groups, _, local = excess.shape
    half = rows // 2
    member = g.tp
    partner = {"rep": g.rep, "fs": g.place, "tp": 1 - member}

    def pair_copy(kind, index, source, target):
        return pltpu.make_async_remote_copy(
            src_ref=source.at[index],
            dst_ref=target.at[index],
            send_sem=pair_send.at[kind, index],
            recv_sem=pair_recv.at[kind, index],
            device_id=partner,
            device_id_type=pl.DeviceIdType.MESH,
        )

    def excess_copy(group):
        return pair_copy(0, group, excess, excess_in)

    def merged_copy(group):
        return pair_copy(1, group, merged, merged_in)

    def part_copy(k):
        return pair_copy(2, k, part_out, part_in)

    def norm_in():
        @pl.loop(0, rows // 16)
        def _(i):
            at = pl.ds(pl.multiple_of(i * 16, 16), 16)
            normed[at, :] = norm_rows(tokens[at, :], mixer_gain[...]).astype(jnp.bfloat16)

    def value_piece(group):
        cut = pl.ds(group * local, local)
        value = jnp.dot(normed[...], fulls[VALUE][:, cut], preferred_element_type=jnp.float32) * value_scale[:, cut]
        floats = value.astype(jnp.bfloat16).astype(jnp.float32)
        place = lax.broadcasted_iota(jnp.int32, floats.shape, 0)
        running = floats
        for level in range(group + 1):
            shifted = pltpu.roll(running, 2**level, 0)
            running = running + jnp.where(place >= 2**level, shifted, 0.0)
        counts = jnp.minimum(place + 1, 2 ** (group + 1)).astype(jnp.float32)
        excess[group] = (running / counts - floats).astype(jnp.bfloat16)
        excess_copy(group).start()

    def gate_piece(group):
        cut = pl.ds(group * local, local)

        @pl.loop(0, 2)
        def _(i):
            at = pl.ds(pl.multiple_of(i * half, half), half)
            value = jnp.dot(normed[at, :], fulls[GATE][:, cut], preferred_element_type=jnp.float32)
            gate[group, at, :] = jax.nn.sigmoid(value * gate_scale[:, cut])

    def pool_piece(group):
        excess_copy(group).wait_recv()
        weight = fulls[POOL].at[group]
        mine = weight[pl.ds(pl.multiple_of(member * local, local), local), :]
        theirs = weight[pl.ds(pl.multiple_of((1 - member) * local, local), local), :]
        pooled = jnp.dot(excess[group], mine, preferred_element_type=jnp.float32) + jnp.dot(
            excess_in[group], theirs, preferred_element_type=jnp.float32
        )
        scale = pool_scale[:, pl.ds(group * local, local)]
        merged[group] = (gate[group] * (pooled * scale)).astype(jnp.bfloat16)
        merged_copy(group).start()

    def slabs(at):
        for group in range(groups):
            for source, owner in ((merged, member), (merged_in, 1 - member)):
                cut = pl.ds(pl.multiple_of((2 * group + owner) * local, local), local)
                yield cut, tokens[at, cut].astype(jnp.float32) + source[group, at, :].astype(jnp.float32)

    def norm_mid(part, parts):
        if part == 0:
            for group in range(groups):
                merged_copy(group).wait_recv()
        steps = rows // 16 // parts

        @pl.loop(part * steps, (part + 1) * steps)
        def _(i):
            at = pl.ds(pl.multiple_of(i * 16, 16), 16)
            held = list(slabs(at))
            total = sum(jnp.sum(values * values, axis=-1, keepdims=True) for _, values in held)
            factor = lax.rsqrt(total / width + 1e-06)
            for cut, values in held:
                normed[at, cut] = (values * factor * channel_gain[:, cut]).astype(jnp.bfloat16)

    def up_piece(n):
        cut = pl.ds(n * local, local)

        @pl.loop(0, 2)
        def _(i):
            at = pl.ds(pl.multiple_of(i * half, half), half)
            upward = jnp.dot(normed[at, :], fulls[HIDE][:, cut], preferred_element_type=jnp.float32) * up_scale[:, cut]
            hidden[at, cut] = jnp.square(jax.nn.relu(upward)).astype(jnp.bfloat16)

    inner = hidden.shape[1]

    def down_piece(k, first):
        weight = fulls[SHOW][pl.ds(pl.multiple_of(k * inner, inner), inner), :]
        scale = fulls[SCALES][pl.ds(pl.multiple_of(k * 16, 16), 16), :][:1]
        at = pl.ds(pl.multiple_of(first, half), half)
        part = jnp.dot(hidden[at, :], weight, preferred_element_type=jnp.float32) * scale
        return part.astype(jnp.bfloat16)

    def finish():
        wide = fulls[SHOW].shape[1]

        @pl.loop(0, g.nf)
        def _(k):
            part_out[k] = down_piece(k, (1 - member) * half)
            part_copy(k).start()

        @pl.loop(0, g.nf)
        def _(k):
            part_own[k] = down_piece(k, member * half)

        @pl.loop(0, g.nf)
        def _(k):
            part_copy(k).wait_recv()

        @pl.loop(0, g.nf)
        def _(k):
            cut = pl.ds(pl.multiple_of(k * wide, wide), wide)
            summed = part_own[k].astype(jnp.float32) + part_in[k].astype(jnp.float32)
            out[:, cut] = (middle_of(k) + summed).astype(out.dtype)

    def middle_of(k):
        group, owner = k // 2, k % 2
        cut = pl.ds(pl.multiple_of(k * local, local), local)
        at = pl.ds(pl.multiple_of(member * half, half), half)
        own = merged[group, at, :].astype(jnp.float32)
        other = merged_in[group, at, :].astype(jnp.float32)
        return tokens[at, cut].astype(jnp.float32) + jnp.where(owner == member, own, other)

    work = []

    def emit(n):
        for _ in range(min(n, len(work))):
            work.pop(0)()

    def queue(w):
        g.ready(w)
        if w == VALUE:
            work.extend(functools.partial(value_piece, i) for i in range(groups))
        elif w == GATE:
            work.extend(functools.partial(gate_piece, i) for i in range(groups))
        elif w == SCALES:
            work.extend(functools.partial(pool_piece, i) for i in range(groups))
            work.extend(functools.partial(norm_mid, i, 3) for i in range(3))
        elif w == HIDE:
            work.extend(functools.partial(up_piece, i) for i in range(inner // local))

    for w in range(count):
        g.local(w).start()
    g.barrier((partner,))
    for w in range(count):
        g.local(w).wait()
    g.own(0)
    norm_in()
    for w in range(count):
        for d in range(1, g.nz):
            g.along(w, d)
            if d == 1:
                if w + 1 < count:
                    g.own(w + 1)
                if w:
                    g.across(w - 1, g.nz - 1)
                    queue(w - 1)
            else:
                g.across(w, d - 2)
            emit(2)
        g.across(w, g.nz - 2)
        emit(2)
    g.across(count - 1, g.nz - 1)
    emit(len(work))
    g.ready(count - 1)
    finish()
    for group in range(groups):
        excess_copy(group).wait_send()
        merged_copy(group).wait_send()

    @pl.loop(0, g.nf)
    def _(k):
        part_copy(k).wait_send()

    g.drain()


def run_layer(sizes, tokens, vectors, weights):
    rows, width = tokens.shape
    count = len(weights)
    fulls = []
    for weight, axis in zip(weights, AXES):
        shape = list(weight.shape)
        shape[axis] *= sizes["fs"]
        fulls.append(pltpu.VMEM(tuple(shape), weight.dtype))
    groups, _, local = weights[POOL].shape
    inner, wide = weights[SHOW].shape
    halves = (sizes["fs"], rows // 2, wide)
    pieces = (groups, rows, local)
    return pl.pallas_call(
        functools.partial(layer_kernel, sizes),
        out_shape=jax.ShapeDtypeStruct((rows // 2, width), jnp.bfloat16),
        in_specs=[pl.BlockSpec(memory_space=pltpu.VMEM)] * (1 + len(vectors))
        + [pl.BlockSpec(memory_space=pl.ANY)] * count,
        out_specs=pl.BlockSpec(memory_space=pltpu.VMEM),
        scratch_shapes=fulls
        + [
            pltpu.VMEM((rows, width), jnp.bfloat16),
            pltpu.VMEM(pieces, jnp.bfloat16),
            pltpu.VMEM(pieces, jnp.bfloat16),
            pltpu.VMEM(pieces, jnp.float32),
            pltpu.VMEM(pieces, jnp.bfloat16),
            pltpu.VMEM(pieces, jnp.bfloat16),
            pltpu.VMEM((rows, inner), jnp.bfloat16),
            pltpu.VMEM(halves, jnp.bfloat16),
            pltpu.VMEM(halves, jnp.bfloat16),
            pltpu.VMEM(halves, jnp.bfloat16),
            pltpu.SemaphoreType.DMA((4, count, sizes["fs"])),
            pltpu.SemaphoreType.DMA((2, count, sizes["fs"])),
            pltpu.SemaphoreType.DMA((count,)),
            pltpu.SemaphoreType.DMA((3, 8)),
            pltpu.SemaphoreType.DMA((3, 8)),
        ],
        compiler_params=pltpu.CompilerParams(
            collective_id=0, has_side_effects=True, vmem_limit_bytes=63 * 2**20
        ),
    )(tokens, *vectors, *weights)


def norm_rows(values, gain):
    floats = values.astype(jnp.float32)
    return floats * lax.rsqrt(jnp.mean(floats * floats, axis=-1, keepdims=True) + 1e-06) * gain


def pool_excess(value):
    floats = value.astype(jnp.float32)
    seq_length = floats.shape[1]
    running = floats
    results = []
    for group in range(floats.shape[2]):
        span = 2**group
        shifted = jnp.pad(running, ((0, 0), (span, 0), (0, 0), (0, 0)))[:, :seq_length]
        running = running + shifted
        counts = jnp.minimum(jnp.arange(1, seq_length + 1), 2 * span).astype(jnp.float32)
        results.append(running[:, :, group, :] / counts[None, :, None] - floats[:, :, group, :])
    return jnp.stack(results, axis=2)


def per_device(
    tokens,
    mixer_gain,
    value_weight,
    value_scale,
    gate_weight,
    gate_scale,
    pool_weight,
    pool_scale,
    channel_gain,
    up_weight,
    up_scale,
    down_weight,
    down_scale,
):
    seq_count, seq_length, model_width = tokens.shape
    shares = lax.axis_size("tp")
    member = lax.axis_index("tp")
    kept_rows = seq_length // shares
    row_count = seq_count * seq_length
    group_count, local_width = value_scale.shape
    value_full, gate_full, pool_full = (
        lax.all_gather(value_weight.astype(jnp.bfloat16), "fs", axis=0, tiled=True),
        lax.all_gather(gate_weight.astype(jnp.bfloat16), "fs", axis=0, tiled=True),
        lax.all_gather(pool_weight.astype(jnp.bfloat16), "fs", axis=1, tiled=True),
    )
    down_scales = lax.all_gather(down_scale, "fs", axis=0, tiled=True)
    normed = norm_rows(tokens, mixer_gain).astype(jnp.bfloat16).reshape(row_count, model_width)
    value = jnp.dot(normed, value_full.reshape(model_width, -1), preferred_element_type=jnp.float32)
    value = (
        (value * value_scale.reshape(-1))
        .astype(jnp.bfloat16)
        .reshape(seq_count, seq_length, group_count, local_width)
    )
    gating = jnp.dot(normed, gate_full.reshape(model_width, -1), preferred_element_type=jnp.float32)
    gating = (gating * gate_scale.reshape(-1)).reshape(
        seq_count, seq_length, group_count, local_width
    )
    excess = pool_excess(value).astype(jnp.bfloat16)
    rows_part = pool_full
    pooled = jnp.einsum(
        "slgc,gce->slge",
        lax.all_gather(excess, "tp", axis=3, tiled=True),
        rows_part,
        preferred_element_type=jnp.float32,
    )
    merged = (jax.nn.sigmoid(gating) * (pooled * pool_scale)).astype(jnp.bfloat16)
    merged_own = lax.all_to_all(merged, "tp", split_axis=1, concat_axis=3, tiled=True)
    own_rows = lax.dynamic_slice_in_dim(tokens, member * kept_rows, kept_rows, 1)
    middle = own_rows.reshape(seq_count * kept_rows, model_width).astype(
        jnp.float32
    ) + merged_own.reshape(seq_count * kept_rows, model_width).astype(jnp.float32)
    normed_two = norm_rows(middle, channel_gain).astype(jnp.bfloat16)
    up_full, down_full = (
        lax.all_gather(up_weight.astype(jnp.bfloat16), "fs", axis=0, tiled=True),
        lax.all_gather(down_weight.astype(jnp.bfloat16), "fs", axis=1, tiled=True),
    )
    upward = (
        jnp.dot(
            lax.all_gather(normed_two, "tp", axis=0, tiled=True),
            up_full,
            preferred_element_type=jnp.float32,
        )
        * up_scale
    )
    hidden = jnp.square(jax.nn.relu(upward)).astype(jnp.bfloat16)
    rows_part = hidden
    summed = lax.psum_scatter(
        (jnp.dot(rows_part, down_full, preferred_element_type=jnp.float32) * down_scales).astype(
            jnp.bfloat16
        ),
        "tp",
        scatter_dimension=0,
        tiled=True,
    ).astype(jnp.float32)
    return (middle + summed).astype(jnp.bfloat16).reshape(seq_count, kept_rows, model_width)


def paired_device(
    sizes,
    tokens,
    mixer_gain,
    value_weight,
    value_scale,
    gate_weight,
    gate_scale,
    pool_weight,
    pool_scale,
    channel_gain,
    up_weight,
    up_scale,
    down_weight,
    down_scale,
):
    rows = value_weight.shape[0]
    row = lambda vector: vector.reshape(1, -1)
    out = run_layer(
        sizes,
        tokens[0],
        (
            row(mixer_gain),
            row(value_scale),
            row(gate_scale),
            row(pool_scale),
            row(channel_gain),
            row(up_scale),
        ),
        (
            value_weight.astype(jnp.bfloat16).reshape(rows, -1),
            gate_weight.astype(jnp.bfloat16).reshape(rows, -1),
            pool_weight.astype(jnp.bfloat16),
            jnp.broadcast_to(row(down_scale), (16, down_scale.shape[0])),
            up_weight.astype(jnp.bfloat16),
            down_weight.astype(jnp.bfloat16),
        ),
    )
    return out[None]


def solution(mesh):
    sizes = dict(mesh.shape)
    paired = sizes["rep"] == 2 and sizes["tp"] == 2 and sizes["fs"] % NY == 0 and sizes["fs"] == 8

    def body(tokens, *rest):
        value_scale, down_scale = rest[2], rest[-1]
        if paired and tokens.shape[0] == 1 and value_scale.shape[1] == down_scale.shape[0]:
            return paired_device(sizes, tokens, *rest)
        return per_device(tokens, *rest)

    return jax.shard_map(
        body,
        mesh=mesh,
        in_specs=(
            P(("rep", "fs"), None, None),
            P(),
            P("fs", None, "tp"),
            P(None, "tp"),
            P("fs", None, "tp"),
            P(None, "tp"),
            P(None, "fs", "tp"),
            P(None, "tp"),
            P(),
            P("fs", "tp"),
            P("tp"),
            P("tp", "fs"),
            P("fs"),
        ),
        out_specs=P(("rep", "fs"), "tp", None),
        check_vma=False,
    )
```

```python
import functools

import jax
import jax.numpy as jnp
from jax import lax
from jax.experimental import pallas as pl
from jax.experimental.pallas import tpu as pltpu
from jax.sharding import PartitionSpec as P

NY = 2
UP, DOWN, ACROSS, SIBLING = range(4)


class Gather:
    def __init__(self, sizes, srcs, fulls, axes, send_sem, recv_sem, local_sem):
        self.nf = sizes["fs"]
        self.nz = self.nf // NY
        self.rep, self.place, self.tp = lax.axis_index("rep"), lax.axis_index("fs"), lax.axis_index("tp")
        self.z, self.y = self.place // NY, self.place % NY
        self.srcs, self.fulls, self.axes = srcs, fulls, axes
        self.send_sem, self.recv_sem, self.local_sem = send_sem, recv_sem, local_sem

    def target(self, way):
        rep, place = self.rep, self.place
        if way == UP:
            place = place + NY
        elif way == DOWN:
            place = place - NY
        elif way == ACROSS:
            place = self.z * NY + 1 - self.y
        else:
            rep = 1 - rep
        return {"rep": rep, "fs": place, "tp": self.tp}

    def view(self, ref, w, start, size):
        axis = self.axes[w]
        return ref.at[tuple([slice(None)] * axis + [pl.ds(start, size)])]

    def piece(self, w, k, half):
        rows = self.srcs[w].shape[self.axes[w]]
        part = rows // 2
        start = pl.multiple_of(k * rows + half * part, part)
        return self.view(self.fulls[w], w, start, part)

    def copy(self, w, k, way, half=None):
        half = self.rep if half is None else half
        return pltpu.make_async_remote_copy(
            src_ref=self.piece(w, k, half),
            dst_ref=self.piece(w, k, half),
            send_sem=self.send_sem.at[way, w, k],
            recv_sem=self.recv_sem.at[1 if way == SIBLING else 0, w, k],
            device_id=self.target(way),
            device_id_type=pl.DeviceIdType.MESH,
        )

    def barrier(self, others=()):
        sem = pltpu.get_barrier_semaphore()

        def greet(device):
            pl.semaphore_signal(sem, inc=1, device_id=device, device_id_type=pl.DeviceIdType.MESH)

        for way in (ACROSS, SIBLING):
            greet(self.target(way))
        for device in others:
            greet(device)
        pl.when(self.z > 0)(lambda: greet(self.target(DOWN)))
        pl.when(self.z < self.nz - 1)(lambda: greet(self.target(UP)))
        ends = (self.z > 0).astype(jnp.int32) + (self.z < self.nz - 1).astype(jnp.int32)
        pl.semaphore_wait(sem, 2 + len(others) + ends)

    def local(self, w):
        rows = self.srcs[w].shape[self.axes[w]]
        return pltpu.make_async_copy(
            self.srcs[w], self.view(self.fulls[w], w, pl.multiple_of(self.place * rows, rows), rows), self.local_sem.at[w]
        )

    def own(self, w):
        pl.when(self.z < self.nz - 1)(lambda: self.copy(w, self.place, UP).start())
        pl.when(self.z > 0)(lambda: self.copy(w, self.place, DOWN).start())
        self.copy(w, self.place, ACROSS).start()

    def pass_on(self, w, k, ways):
        self.copy(w, k, ACROSS).wait_recv()
        for way in ways:
            if way == UP:
                pl.when(self.z < self.nz - 1)(lambda: self.copy(w, k, UP).start())
            elif way == DOWN:
                pl.when(self.z > 0)(lambda: self.copy(w, k, DOWN).start())
            else:
                self.copy(w, k, way).start()

    def along(self, w, d):
        pl.when(self.z >= d)(lambda: self.pass_on(w, (self.z - d) * NY + self.y, (UP, ACROSS, SIBLING)))
        pl.when(self.z + d < self.nz)(lambda: self.pass_on(w, (self.z + d) * NY + self.y, (DOWN, ACROSS, SIBLING)))

    def across(self, w, d):
        other = 1 - self.y
        pl.when(self.z >= d)(lambda: self.pass_on(w, (self.z - d) * NY + other, (SIBLING,)))
        if d:
            pl.when(self.z + d < self.nz)(lambda: self.pass_on(w, (self.z + d) * NY + other, (SIBLING,)))

    def ready(self, w):
        @pl.loop(0, self.nf)
        def _(k):
            pl.when(k != self.place)(lambda: self.copy(w, k, SIBLING, half=1 - self.rep).wait_recv())

    def nearest(self, i):
        ends = self.nz - 1 - self.z
        short = jnp.minimum(self.z, ends)
        near = self.z - (i + 1) // 2 if i % 2 else self.z + i // 2
        far = jnp.where(self.z < ends, self.z + (i - short), self.z - (i - short))
        return jnp.where(i <= 2 * short, near, far)

    def drain(self):
        for w in range(len(self.srcs)):

            @pl.loop(0, self.nf)
            def _(k):
                z, y = k // NY, k % NY
                mine = y == self.y
                pl.when(mine & (z <= self.z) & (self.z < self.nz - 1))(lambda: self.copy(w, k, UP).wait_send())
                pl.when(mine & (z >= self.z) & (self.z > 0))(lambda: self.copy(w, k, DOWN).wait_send())
                pl.when(mine)(lambda: self.copy(w, k, ACROSS).wait_send())
                pl.when(k != self.place)(lambda: self.copy(w, k, SIBLING).wait_send())


VALUE, GATE, POOL, SCALES, HIDE, SHOW = range(6)
AXES = (0, 0, 1, 0, 0, 0)


def layer_kernel(sizes, *refs):
    count = len(AXES)
    tokens, mixer_gain, value_scale, gate_scale, pool_scale, channel_gain, up_scale = refs[:7]
    srcs, out, fulls = refs[7 : 7 + count], refs[7 + count], refs[8 + count : 8 + 2 * count]
    normed, excess, excess_in, gate, merged, merged_in, hidden, part_out, part_own, part_in = refs[
        8 + 2 * count : 18 + 2 * count
    ]
    send_sem, recv_sem, local_sem, pair_send, pair_recv = refs[18 + 2 * count :]
    g = Gather(sizes, srcs, fulls, AXES, send_sem, recv_sem, local_sem)
    rows, width = tokens.shape
    groups, _, local = excess.shape
    half = rows // 2
    member = g.tp
    partner = {"rep": g.rep, "fs": g.place, "tp": 1 - member}

    def pair_copy(kind, index, source, target):
        return pltpu.make_async_remote_copy(
            src_ref=source.at[index],
            dst_ref=target.at[index],
            send_sem=pair_send.at[kind, index],
            recv_sem=pair_recv.at[kind, index],
            device_id=partner,
            device_id_type=pl.DeviceIdType.MESH,
        )

    def excess_copy(group):
        return pair_copy(0, group, excess, excess_in)

    def merged_copy(group):
        return pair_copy(1, group, merged, merged_in)

    def part_copy(k):
        return pair_copy(2, k, part_out, part_in)

    def norm_in():
        @pl.loop(0, rows // 16)
        def _(i):
            at = pl.ds(pl.multiple_of(i * 16, 16), 16)
            normed[at, :] = norm_rows(tokens[at, :], mixer_gain[...]).astype(jnp.bfloat16)

    def value_piece(group):
        cut = pl.ds(group * local, local)
        value = jnp.dot(normed[...], fulls[VALUE][:, cut], preferred_element_type=jnp.float32) * value_scale[group : group + 1]
        floats = value.astype(jnp.bfloat16).astype(jnp.float32)
        place = lax.broadcasted_iota(jnp.int32, floats.shape, 0)
        running = floats
        for level in range(group + 1):
            shifted = pltpu.roll(running, 2**level, 0)
            running = running + jnp.where(place >= 2**level, shifted, 0.0)
        counts = jnp.minimum(place + 1, 2 ** (group + 1)).astype(jnp.float32)
        excess[group] = (running / counts - floats).astype(jnp.bfloat16)
        excess_copy(group).start()

    def gate_piece(group):
        cut = pl.ds(group * local, local)

        @pl.loop(0, 2)
        def _(i):
            at = pl.ds(pl.multiple_of(i * half, half), half)
            value = jnp.dot(normed[at, :], fulls[GATE][:, cut], preferred_element_type=jnp.float32)
            gate[group, at, :] = jax.nn.sigmoid(value * gate_scale[group : group + 1])

    def pool_piece(group):
        excess_copy(group).wait_recv()
        weight = fulls[POOL].at[group]
        mine = weight[pl.ds(pl.multiple_of(member * local, local), local), :]
        theirs = weight[pl.ds(pl.multiple_of((1 - member) * local, local), local), :]
        pooled = jnp.dot(excess[group], mine, preferred_element_type=jnp.float32) + jnp.dot(
            excess_in[group], theirs, preferred_element_type=jnp.float32
        )
        scale = pool_scale[group : group + 1]
        merged[group] = (gate[group] * (pooled * scale)).astype(jnp.bfloat16)
        merged_copy(group).start()

    def slabs(at):
        for group in range(groups):
            for source, owner in ((merged, member), (merged_in, 1 - member)):
                cut = pl.ds(pl.multiple_of((2 * group + owner) * local, local), local)
                yield cut, tokens[at, cut].astype(jnp.float32) + source[group, at, :].astype(jnp.float32)

    def norm_mid(part, parts):
        if part == 0:
            for group in range(groups):
                merged_copy(group).wait_recv()
        steps = rows // 16 // parts

        @pl.loop(part * steps, (part + 1) * steps)
        def _(i):
            at = pl.ds(pl.multiple_of(i * 16, 16), 16)
            held = list(slabs(at))
            total = sum(jnp.sum(values * values, axis=-1, keepdims=True) for _, values in held)
            factor = lax.rsqrt(total / width + 1e-06)
            for cut, values in held:
                normed[at, cut] = (values * factor * channel_gain[:, cut]).astype(jnp.bfloat16)

    def up_piece(n):
        cut = pl.ds(n * local, local)

        @pl.loop(0, 2)
        def _(i):
            at = pl.ds(pl.multiple_of(i * half, half), half)
            upward = jnp.dot(normed[at, :], fulls[HIDE][:, cut], preferred_element_type=jnp.float32) * up_scale[:, cut]
            hidden[at, cut] = jnp.square(jax.nn.relu(upward)).astype(jnp.bfloat16)

    inner = hidden.shape[1]

    def down_piece(k, first):
        weight = fulls[SHOW][pl.ds(pl.multiple_of(k * inner, inner), inner), :]
        scale = fulls[SCALES][pl.ds(pl.multiple_of(k * 16, 16), 16), :][:1]
        at = pl.ds(pl.multiple_of(first, half), half)
        part = jnp.dot(hidden[at, :], weight, preferred_element_type=jnp.float32) * scale
        return part.astype(jnp.bfloat16)

    def down_step(i, y):
        k = g.nearest(i) * NY + y
        if i or y is not g.y:
            g.copy(SHOW, k, SIBLING, half=1 - g.rep).wait_recv()
        part_out[k] = down_piece(k, (1 - member) * half)
        part_copy(k).start()
        part_own[k] = down_piece(k, member * half)

    def finish():
        wide = fulls[SHOW].shape[1]

        @pl.loop(0, g.nf)
        def _(k):
            part_copy(k).wait_recv()
            cut = pl.ds(pl.multiple_of(k * wide, wide), wide)
            summed = part_own[k].astype(jnp.float32) + part_in[k].astype(jnp.float32)
            out[:, cut] = (middle_of(k) + summed).astype(out.dtype)

    def middle_of(k):
        group, owner = k // 2, k % 2
        cut = pl.ds(pl.multiple_of(k * local, local), local)
        at = pl.ds(pl.multiple_of(member * half, half), half)
        own = merged[group, at, :].astype(jnp.float32)
        other = merged_in[group, at, :].astype(jnp.float32)
        return tokens[at, cut].astype(jnp.float32) + jnp.where(owner == member, own, other)

    work = []

    def emit(n):
        for _ in range(min(n, len(work))):
            work.pop(0)()

    def queue(w):
        g.ready(w)
        if w == VALUE:
            work.extend(functools.partial(value_piece, i) for i in range(groups))
        elif w == GATE:
            work.extend(functools.partial(gate_piece, i) for i in range(groups))
        elif w == SCALES:
            work.extend(functools.partial(pool_piece, i) for i in range(groups))
            work.extend(functools.partial(norm_mid, i, 3) for i in range(3))
        elif w == HIDE:
            work.extend(functools.partial(up_piece, i) for i in range(inner // local))

    other = 1 - g.y
    for w in range(count):
        g.local(w).start()
    g.barrier((partner,))
    for w in range(count):
        g.local(w).wait()
    g.own(0)
    norm_in()
    for w in range(count):
        for d in range(1, g.nz):
            g.along(w, d)
            if d == 1:
                if w + 1 < count:
                    g.own(w + 1)
                if w:
                    g.across(w - 1, g.nz - 1)
                    queue(w - 1)
                    if w == SHOW:
                        work.append(functools.partial(down_step, 0, g.y))
            else:
                g.across(w, d - 2)
            if w == SHOW:
                work.append(functools.partial(down_step, d, g.y))
                if d > 1:
                    work.append(functools.partial(down_step, d - 2, other))
            emit(4 if w == SHOW else 2)
        g.across(w, g.nz - 2)
        if w == SHOW:
            work.append(functools.partial(down_step, g.nz - 2, other))
        emit(4 if w == SHOW else 2)
    emit(len(work))
    g.across(count - 1, g.nz - 1)
    down_step(g.nz - 1, other)
    finish()
    for group in range(groups):
        excess_copy(group).wait_send()
        merged_copy(group).wait_send()

    @pl.loop(0, g.nf)
    def _(k):
        part_copy(k).wait_send()

    g.drain()


def run_layer(sizes, tokens, vectors, weights):
    rows, width = tokens.shape
    count = len(weights)
    fulls = []
    for weight, axis in zip(weights, AXES):
        shape = list(weight.shape)
        shape[axis] *= sizes["fs"]
        fulls.append(pltpu.VMEM(tuple(shape), weight.dtype))
    groups, _, local = weights[POOL].shape
    inner, wide = weights[SHOW].shape
    halves = (sizes["fs"], rows // 2, wide)
    pieces = (groups, rows, local)
    return pl.pallas_call(
        functools.partial(layer_kernel, sizes),
        out_shape=jax.ShapeDtypeStruct((rows // 2, width), jnp.bfloat16),
        in_specs=[pl.BlockSpec(memory_space=pltpu.VMEM)] * (1 + len(vectors))
        + [pl.BlockSpec(memory_space=pl.ANY)] * count,
        out_specs=pl.BlockSpec(memory_space=pltpu.VMEM),
        scratch_shapes=fulls
        + [
            pltpu.VMEM((rows, width), jnp.bfloat16),
            pltpu.VMEM(pieces, jnp.bfloat16),
            pltpu.VMEM(pieces, jnp.bfloat16),
            pltpu.VMEM(pieces, jnp.float32),
            pltpu.VMEM(pieces, jnp.bfloat16),
            pltpu.VMEM(pieces, jnp.bfloat16),
            pltpu.VMEM((rows, inner), jnp.bfloat16),
            pltpu.VMEM(halves, jnp.bfloat16),
            pltpu.VMEM(halves, jnp.bfloat16),
            pltpu.VMEM(halves, jnp.bfloat16),
            pltpu.SemaphoreType.DMA((4, count, sizes["fs"])),
            pltpu.SemaphoreType.DMA((2, count, sizes["fs"])),
            pltpu.SemaphoreType.DMA((count,)),
            pltpu.SemaphoreType.DMA((3, 8)),
            pltpu.SemaphoreType.DMA((3, 8)),
        ],
        compiler_params=pltpu.CompilerParams(
            collective_id=0, has_side_effects=True, vmem_limit_bytes=63 * 2**20
        ),
    )(tokens, *vectors, *weights)


def norm_rows(values, gain):
    floats = values.astype(jnp.float32)
    return floats * lax.rsqrt(jnp.mean(floats * floats, axis=-1, keepdims=True) + 1e-06) * gain


def pool_excess(value):
    floats = value.astype(jnp.float32)
    seq_length = floats.shape[1]
    running = floats
    results = []
    for group in range(floats.shape[2]):
        span = 2**group
        shifted = jnp.pad(running, ((0, 0), (span, 0), (0, 0), (0, 0)))[:, :seq_length]
        running = running + shifted
        counts = jnp.minimum(jnp.arange(1, seq_length + 1), 2 * span).astype(jnp.float32)
        results.append(running[:, :, group, :] / counts[None, :, None] - floats[:, :, group, :])
    return jnp.stack(results, axis=2)


def per_device(
    tokens,
    mixer_gain,
    value_weight,
    value_scale,
    gate_weight,
    gate_scale,
    pool_weight,
    pool_scale,
    channel_gain,
    up_weight,
    up_scale,
    down_weight,
    down_scale,
):
    seq_count, seq_length, model_width = tokens.shape
    shares = lax.axis_size("tp")
    member = lax.axis_index("tp")
    kept_rows = seq_length // shares
    row_count = seq_count * seq_length
    group_count, local_width = value_scale.shape
    value_full, gate_full, pool_full = (
        lax.all_gather(value_weight.astype(jnp.bfloat16), "fs", axis=0, tiled=True),
        lax.all_gather(gate_weight.astype(jnp.bfloat16), "fs", axis=0, tiled=True),
        lax.all_gather(pool_weight.astype(jnp.bfloat16), "fs", axis=1, tiled=True),
    )
    down_scales = lax.all_gather(down_scale, "fs", axis=0, tiled=True)
    normed = norm_rows(tokens, mixer_gain).astype(jnp.bfloat16).reshape(row_count, model_width)
    value = jnp.dot(normed, value_full.reshape(model_width, -1), preferred_element_type=jnp.float32)
    value = (
        (value * value_scale.reshape(-1))
        .astype(jnp.bfloat16)
        .reshape(seq_count, seq_length, group_count, local_width)
    )
    gating = jnp.dot(normed, gate_full.reshape(model_width, -1), preferred_element_type=jnp.float32)
    gating = (gating * gate_scale.reshape(-1)).reshape(
        seq_count, seq_length, group_count, local_width
    )
    excess = pool_excess(value).astype(jnp.bfloat16)
    rows_part = pool_full
    pooled = jnp.einsum(
        "slgc,gce->slge",
        lax.all_gather(excess, "tp", axis=3, tiled=True),
        rows_part,
        preferred_element_type=jnp.float32,
    )
    merged = (jax.nn.sigmoid(gating) * (pooled * pool_scale)).astype(jnp.bfloat16)
    merged_own = lax.all_to_all(merged, "tp", split_axis=1, concat_axis=3, tiled=True)
    own_rows = lax.dynamic_slice_in_dim(tokens, member * kept_rows, kept_rows, 1)
    middle = own_rows.reshape(seq_count * kept_rows, model_width).astype(
        jnp.float32
    ) + merged_own.reshape(seq_count * kept_rows, model_width).astype(jnp.float32)
    normed_two = norm_rows(middle, channel_gain).astype(jnp.bfloat16)
    up_full, down_full = (
        lax.all_gather(up_weight.astype(jnp.bfloat16), "fs", axis=0, tiled=True),
        lax.all_gather(down_weight.astype(jnp.bfloat16), "fs", axis=1, tiled=True),
    )
    upward = (
        jnp.dot(
            lax.all_gather(normed_two, "tp", axis=0, tiled=True),
            up_full,
            preferred_element_type=jnp.float32,
        )
        * up_scale
    )
    hidden = jnp.square(jax.nn.relu(upward)).astype(jnp.bfloat16)
    rows_part = hidden
    summed = lax.psum_scatter(
        (jnp.dot(rows_part, down_full, preferred_element_type=jnp.float32) * down_scales).astype(
            jnp.bfloat16
        ),
        "tp",
        scatter_dimension=0,
        tiled=True,
    ).astype(jnp.float32)
    return (middle + summed).astype(jnp.bfloat16).reshape(seq_count, kept_rows, model_width)


def paired_device(
    sizes,
    tokens,
    mixer_gain,
    value_weight,
    value_scale,
    gate_weight,
    gate_scale,
    pool_weight,
    pool_scale,
    channel_gain,
    up_weight,
    up_scale,
    down_weight,
    down_scale,
):
    rows = value_weight.shape[0]
    row = lambda vector: vector.reshape(1, -1)
    out = run_layer(
        sizes,
        tokens[0],
        (
            row(mixer_gain),
            value_scale,
            gate_scale,
            pool_scale,
            row(channel_gain),
            row(up_scale),
        ),
        (
            value_weight.astype(jnp.bfloat16).reshape(rows, -1),
            gate_weight.astype(jnp.bfloat16).reshape(rows, -1),
            pool_weight.astype(jnp.bfloat16),
            jnp.broadcast_to(row(down_scale), (16, down_scale.shape[0])),
            up_weight.astype(jnp.bfloat16),
            down_weight.astype(jnp.bfloat16),
        ),
    )
    return out[None]


def solution(mesh):
    sizes = dict(mesh.shape)
    paired = sizes["rep"] == 2 and sizes["tp"] == 2 and sizes["fs"] % NY == 0 and sizes["fs"] == 8

    def body(tokens, *rest):
        value_scale, down_scale = rest[2], rest[-1]
        if paired and tokens.shape[0] == 1 and value_scale.shape[1] == down_scale.shape[0]:
            return paired_device(sizes, tokens, *rest)
        return per_device(tokens, *rest)

    return jax.shard_map(
        body,
        mesh=mesh,
        in_specs=(
            P(("rep", "fs"), None, None),
            P(),
            P("fs", None, "tp"),
            P(None, "tp"),
            P("fs", None, "tp"),
            P(None, "tp"),
            P(None, "fs", "tp"),
            P(None, "tp"),
            P(),
            P("fs", "tp"),
            P("tp"),
            P("tp", "fs"),
            P("fs"),
        ),
        out_specs=P(("rep", "fs"), "tp", None),
        check_vma=False,
    )
```
